32 devices in a mesh: rep: 2 (over x), fs: 8 (over z, y), tp: 2 (over core).
Axes of the slice: x: 2, y: 2, z: 4, core: 2. Of those that a mesh axis runs over, the one named last changes fastest.
Arguments:
- tokens: bfloat16 [12288, 2048], P(('rep', 'fs'), 'tp'), may hold values from -6 to 6
- first_norm_gain: bfloat16 [2048], replicated, may hold values from 0.099609375 to 1.8984375
- query_projection_weight: bfloat16 [2048, 512], P('fs', 'tp'), may hold values from -0.125 to 0.125
- key_projection_weight: bfloat16 [2048, 512], P('fs', 'tp'), may hold values from -0.125 to 0.125
- value_projection_weight: bfloat16 [2048, 1024], P('fs', 'tp'), may hold values from -0.125 to 0.125
- output_gate_weight: bfloat16 [2048, 1024], P('fs', 'tp'), may hold values from -0.125 to 0.125
- decay_projection_weight: bfloat16 [2048, 512], P('fs', 'tp'), may hold values from -0.375 to 0.375
- fading_shift_vector: float32 [512], P('tp'), may hold values from -1 to 4
- added_fading_exponent: float32 [12288, 512], P(('rep', 'fs'), 'tp'), may hold values from -0.7 to 0
- per_head_gain: bfloat16 [128], replicated, may hold values from 0.099609375 to 1.8984375
- mixer_result_matrix: bfloat16 [1024, 2048], P('tp', 'fs'), may hold values from -0.1875 to 0.1875
- second_norm_gain: bfloat16 [2048], replicated, may hold values from 0.099609375 to 1.8984375
- up_linear_weight: bfloat16 [2048, 3072], P('fs', 'tp'), may hold values from -0.125 to 0.125
- up_gating_weight: bfloat16 [2048, 3072], P('fs', 'tp'), may hold values from -0.125 to 0.125
- depthwise_taps: bfloat16 [2, 3, 3072], P(None, None, 'tp'), may hold values from -3.5 to 3.5
- depthwise_bias: bfloat16 [2, 3072], P(None, 'tp'), may hold values from -3 to 3
- down_projection_weight: bfloat16 [3072, 2048], P('tp', 'fs'), may hold values from -0.109375 to 0.109375
Outputs:
- mixed: bfloat16 [12288, 2048], P(('rep', 'fs'), 'tp')
The draws below stay inside these ranges and needn't reach their ends.
All inputs are finite; a program needn't handle non-finite values.
Results may differ from the reference program's by a relative error of at most 0.018.
Values may be sent and summed in bfloat16 or wider, within the bound.
No kernel may reach another device: no remote copies, remote signals or barrier semaphores. Data moves between devices by JAX's collectives and lax.ppermute only.
A program may use at most 128 MiB of HBM per device.

```python
import math
import jax
import jax.numpy as jnp
from jax import lax

D = 2048
HEADS = 8
KEY_DIM = 64
VALUE_DIM = 128
FF = 3072
KERNEL = 3
BLOCK = 64
SEQ_LEN = 256
TOKENS = 12288
N_TP = 2


def draw_added_fading_exponent(key, part):
    place_key, level_key = jax.random.split(jax.random.fold_in(key, 7))
    struck = jax.random.randint(place_key, (TOKENS, 1), 0, 64) == 0
    strength = jax.random.uniform(level_key, (TOKENS, HEADS * KEY_DIM), jnp.float32, math.log(0.5), math.log(0.8))
    return jnp.where(struck, strength, 0.0).astype(jnp.float32)


def levels(own_key, extent, pieces, smallest, largest):
    def one(dim, blocks):
        steps = jax.random.uniform(jax.random.fold_in(jax.random.fold_in(own_key, 6), dim), (blocks,), jnp.float32, smallest / len(pieces), largest / len(pieces))
        return jnp.repeat(jnp.exp(steps), extent[dim] // blocks).reshape((-1,) + (1,) * (len(extent) - dim - 1))

    level = one(*pieces[0])
    for cut in pieces[1:]:
        level = level * one(*cut)
    return level


def noise(stream_key, extent, deviation, most, cuts=(), kind=jnp.bfloat16):
    factor_of = levels(stream_key, extent, cuts, -0.22, 0.18) if cuts else 1.0
    drawn = jax.random.normal(stream_key, extent, jnp.float32) * deviation * factor_of
    return jnp.minimum(jnp.maximum(drawn, -most), most).astype(kind)


def setup_inputs(seed: int = 0) -> dict:
    key_list = jax.random.split(jax.random.key(seed), 18)
    tokens = noise(key_list[0], (TOKENS, D), 1.0, 6.0, ((0, 16), (1, 2)))
    first_norm_gain = jnp.clip(1.0 + 0.18 * jax.random.normal(key_list[1], (D,), jnp.float32), 0.099609375, 1.8984375).astype(jnp.bfloat16)
    query_projection_weight = noise(key_list[2], (D, HEADS * KEY_DIM), D ** -0.5, 0.125, ((0, 8), (1, 2)))
    key_projection_weight = noise(key_list[3], (D, HEADS * KEY_DIM), D ** -0.5, 0.125, ((0, 8), (1, 2)))
    value_projection_weight = noise(key_list[4], (D, HEADS * VALUE_DIM), D ** -0.5, 0.125, ((0, 8), (1, 2)))
    output_gate_weight = noise(key_list[5], (D, HEADS * VALUE_DIM), D ** -0.5, 0.125, ((0, 8), (1, 2)))
    decay_projection_weight = noise(key_list[6], (D, HEADS * KEY_DIM), (D // 9) ** -0.5, 0.375, ((0, 8), (1, 2)))
    fading_shift_vector = jnp.clip(-1.0 + 5.0 * jax.random.uniform(key_list[7], (HEADS * KEY_DIM,), jnp.float32) ** levels(key_list[7], (HEADS * KEY_DIM,), ((0, 2),), -0.2, 0.2), -1.0, 4.0)
    added_fading_exponent = draw_added_fading_exponent(jax.random.fold_in(key_list[17], 71), 0)
    per_head_gain = jnp.clip(1.0 + 0.18 * jax.random.normal(key_list[9], (VALUE_DIM,), jnp.float32), 0.099609375, 1.8984375).astype(jnp.bfloat16)
    mixer_result_matrix = noise(key_list[10], (HEADS * VALUE_DIM, D), (HEADS * VALUE_DIM) ** -0.5, 0.1875, ((0, 2), (1, 8)))
    second_norm_gain = jnp.clip(1.0 + 0.18 * jax.random.normal(key_list[11], (D,), jnp.float32), 0.099609375, 1.8984375).astype(jnp.bfloat16)
    up_linear_weight = noise(key_list[12], (D, FF), D ** -0.5, 0.125, ((0, 8), (1, 2)))
    up_gating_weight = noise(key_list[13], (D, FF), D ** -0.5, 0.125, ((0, 8), (1, 2)))
    depthwise_taps = noise(key_list[14], (2, KERNEL, FF), KERNEL ** -0.5, 3.5, ((2, 2),))
    depthwise_bias = noise(key_list[15], (2, FF), 0.5, 3.0, ((1, 2),))
    down_projection_weight = noise(key_list[16], (FF, D), FF ** -0.5, 0.109375, ((0, 2), (1, 8)))
    return dict(tokens=tokens, first_norm_gain=first_norm_gain, query_projection_weight=query_projection_weight, key_projection_weight=key_projection_weight, value_projection_weight=value_projection_weight, output_gate_weight=output_gate_weight, decay_projection_weight=decay_projection_weight, fading_shift_vector=fading_shift_vector, added_fading_exponent=added_fading_exponent, per_head_gain=per_head_gain, mixer_result_matrix=mixer_result_matrix, second_norm_gain=second_norm_gain, up_linear_weight=up_linear_weight, up_gating_weight=up_gating_weight, depthwise_taps=depthwise_taps, depthwise_bias=depthwise_bias, down_projection_weight=down_projection_weight)


norm_eps = 1e-06
fading_sharpness = 16.0

def normalize(source, gain):
    widened = source.astype(jnp.float32)
    scaled = widened * lax.rsqrt(lax.optimization_barrier(jnp.mean(widened * widened, axis=-1, keepdims=True)) + norm_eps)
    return (scaled * gain.astype(jnp.float32)).astype(jnp.bfloat16)

def direction(queries, key_heads, value_heads, fading_exponent):
    sequences, length, head_count, key_depth = queries.shape
    value_depth = value_heads.shape[-1]
    block_count = length // BLOCK
    query_blocks = queries.reshape(sequences, block_count, BLOCK, head_count, key_depth)
    key_blocks = key_heads.reshape(sequences, block_count, BLOCK, head_count, key_depth)
    value_blocks = value_heads.reshape(sequences, block_count, BLOCK, head_count, value_depth)
    cumulative = jnp.cumsum(fading_exponent.reshape(sequences, block_count, BLOCK, head_count, key_depth), axis=2)
    block_total = cumulative[:, :, -1:]
    query_decayed = query_blocks * jnp.exp(cumulative)
    key_inverse = key_blocks * jnp.exp(-cumulative)
    key_carried = key_blocks * jnp.exp(block_total - cumulative)
    lower_mask = jnp.tril(jnp.ones((BLOCK, BLOCK), dtype=bool))
    scores = jnp.einsum('snihd,snjhd->snhij', query_decayed, key_inverse, precision=lax.Precision.HIGHEST)
    scores = jnp.where(lower_mask, scores, 0.0)
    within_block = jnp.einsum('snhij,snjhv->snihv', scores, value_blocks, precision=lax.Precision.HIGHEST)
    increments = jnp.einsum('snchd,snchv->nshdv', key_carried, value_blocks, precision=lax.Precision.HIGHEST)
    carry_decay = jnp.moveaxis(jnp.exp(block_total[:, :, 0]), 1, 0)

    def advance(running, inputs):
        factor, update = inputs
        return (factor[..., None] * running + update, running)
    initial = jnp.zeros((sequences, head_count, key_depth, value_depth), jnp.float32)
    unused, previous = lax.scan(advance, initial, (carry_decay, increments))
    across_blocks = jnp.einsum('snchd,nshdv->snchv', query_decayed, previous, precision=lax.Precision.HIGHEST)
    return (within_block + across_blocks).reshape(sequences, length, head_count, value_depth)

def mixer_heads(queries_raw, keys_raw, values_raw, gates_raw, fading_exponent, per_head_gain):
    row_count = queries_raw.shape[0]
    head_count = values_raw.shape[1] // VALUE_DIM
    key_shape = (row_count // SEQ_LEN, SEQ_LEN, head_count, KEY_DIM)
    value_shape = (row_count // SEQ_LEN, SEQ_LEN, head_count, VALUE_DIM)
    queries = queries_raw.astype(jnp.float32).reshape(key_shape) * KEY_DIM ** (-0.5)
    key_heads = keys_raw.astype(jnp.float32).reshape(key_shape)
    value_heads = values_raw.astype(jnp.float32).reshape(value_shape)
    decay_heads = fading_exponent.reshape(key_shape)
    forward = direction(queries, key_heads, value_heads, decay_heads)
    backward = direction(jnp.flip(queries, 1), jnp.flip(key_heads, 1), jnp.flip(value_heads, 1), jnp.flip(decay_heads, 1))
    attention = forward + jnp.flip(backward, 1)
    scaled = attention * lax.rsqrt(lax.optimization_barrier(jnp.mean(attention * attention, axis=-1, keepdims=True)) + norm_eps)
    scaled = scaled * per_head_gain.astype(jnp.float32)
    merged = scaled.reshape(row_count, head_count * VALUE_DIM)
    return (merged * jax.nn.silu(gates_raw.astype(jnp.float32))).astype(jnp.bfloat16)

def depthwise(linear_out, gated_out, depthwise_taps, depthwise_bias):
    row_count, channels = linear_out.shape

    def smooth(source, taps, offset_bias):
        framed = source.astype(jnp.float32).reshape(row_count // SEQ_LEN, SEQ_LEN, channels)
        tap_count = taps.shape[0]
        leading_zero_fill = tap_count // 2
        padded = jnp.pad(framed, ((0, 0), (leading_zero_fill, tap_count - 1 - leading_zero_fill), (0, 0)))
        result = offset_bias.astype(jnp.float32)
        for shift_index in range(tap_count):
            result = result + padded[:, shift_index:shift_index + SEQ_LEN] * taps[shift_index].astype(jnp.float32)
        return result
    linear_conv = smooth(linear_out, depthwise_taps[0], depthwise_bias[0])
    gate_conv = smooth(gated_out, depthwise_taps[1], depthwise_bias[1])
    return (linear_conv * jax.nn.silu(gate_conv)).astype(jnp.bfloat16).reshape(row_count, channels)

def group_sum(left_side, right_side):
    group_rows = left_side.shape[1] // N_TP
    summed = jnp.zeros((left_side.shape[0], right_side.shape[1]), jnp.float32)
    for member in range(N_TP):
        partial_prod = jnp.dot(left_side[:, member * group_rows:(member + 1) * group_rows], right_side[member * group_rows:(member + 1) * group_rows], preferred_element_type=jnp.float32)
        summed = summed + lax.optimization_barrier(partial_prod.astype(jnp.bfloat16)).astype(jnp.float32)
    return summed

def reference(tokens, first_norm_gain, query_projection_weight, key_projection_weight, value_projection_weight, output_gate_weight, decay_projection_weight, fading_shift_vector, added_fading_exponent, per_head_gain, mixer_result_matrix, second_norm_gain, up_linear_weight, up_gating_weight, depthwise_taps, depthwise_bias, down_projection_weight):
    normed = normalize(tokens, first_norm_gain)
    queries_raw = jnp.dot(normed, query_projection_weight, preferred_element_type=jnp.float32).astype(jnp.bfloat16)
    keys_raw = jnp.dot(normed, key_projection_weight, preferred_element_type=jnp.float32).astype(jnp.bfloat16)
    values_raw = jnp.dot(normed, value_projection_weight, preferred_element_type=jnp.float32).astype(jnp.bfloat16)
    gates_raw = jnp.dot(normed, output_gate_weight, preferred_element_type=jnp.float32).astype(jnp.bfloat16)
    fading_scores_raw = jnp.dot(normed, decay_projection_weight, preferred_element_type=jnp.float32)
    fading_exponent = jax.nn.log_sigmoid(fading_scores_raw + fading_shift_vector) / fading_sharpness + added_fading_exponent
    mixed_heads = mixer_heads(queries_raw, keys_raw, values_raw, gates_raw, fading_exponent, per_head_gain)
    mixer_out = group_sum(mixed_heads, mixer_result_matrix)
    after_mixer = (tokens.astype(jnp.float32) + mixer_out).astype(jnp.bfloat16)
    normed_two = normalize(after_mixer, second_norm_gain)
    linear_out = jnp.dot(normed_two, up_linear_weight, preferred_element_type=jnp.float32).astype(jnp.bfloat16)
    gated_out = jnp.dot(normed_two, up_gating_weight, preferred_element_type=jnp.float32).astype(jnp.bfloat16)
    hidden = depthwise(linear_out, gated_out, depthwise_taps, depthwise_bias)
    channel_out = group_sum(hidden, down_projection_weight)
    return (after_mixer.astype(jnp.float32) + channel_out).astype(jnp.bfloat16)
```

```python
import functools

import jax
import jax.numpy as jnp
from jax import lax
from jax.experimental import pallas as pl
from jax.experimental.pallas import tpu as pltpu
from jax.sharding import PartitionSpec as P

KEY_DIM = 64
VALUE_DIM = 128
BLOCK = 64
SEQ_LEN = 256


norm_eps = 1e-06
fading_sharpness = 16.0


def normalize(source, gain):
    widened = source.astype(jnp.float32)
    scaled = widened * lax.rsqrt(jnp.mean(widened * widened, axis=-1, keepdims=True) + norm_eps)
    return (scaled * gain.astype(jnp.float32)).astype(jnp.bfloat16)


def attention_kernel(projected_ref, added_ref, shift_ref, gain_ref, out_ref):
    length, half = added_ref.shape
    head_count = half // KEY_DIM
    wide = head_count * VALUE_DIM
    block_count = length // BLOCK
    rows = lax.broadcasted_iota(jnp.int32, (BLOCK, BLOCK), 0)
    cols = lax.broadcasted_iota(jnp.int32, (BLOCK, BLOCK), 1)
    lower = rows >= cols
    upper = rows <= cols
    ones_lower = lower.astype(jnp.float32)
    gain = gain_ref[...].astype(jnp.float32)
    shift = shift_ref[...]

    def dot(left, right, dims):
        return lax.dot_general(left, right, (dims, ((), ())), preferred_element_type=jnp.float32)

    def rounded(block, start, size):
        part = projected_ref[block * BLOCK : (block + 1) * BLOCK, start : start + size]
        return part.astype(jnp.bfloat16)

    terms = []
    for block in range(block_count):
        span = slice(block * BLOCK, (block + 1) * BLOCK)
        scores = projected_ref[span, 2 * half + 2 * wide :] + shift
        log_decay = (
            jnp.minimum(scores, 0.0) - jnp.log1p(jnp.exp(-jnp.abs(scores)))
        ) / fading_sharpness + added_ref[span, :]
        forward_sum = lax.dot_general(
            ones_lower,
            log_decay,
            (((1,), (0,)), ((), ())),
            precision=lax.Precision.HIGHEST,
            preferred_element_type=jnp.float32,
        )
        total = forward_sum[BLOCK - 1 : BLOCK]
        rest = total - forward_sum
        backward_sum = rest + log_decay
        queries = rounded(block, 0, half).astype(jnp.float32) * KEY_DIM ** (-0.5)
        keys = rounded(block, half, half).astype(jnp.float32)
        kind = jnp.bfloat16
        terms.append(
            dict(
                total=jnp.exp(total),
                query_forward=(queries * jnp.exp(forward_sum)).astype(kind),
                query_backward=(queries * jnp.exp(backward_sum)).astype(kind),
                key_forward=(keys * jnp.exp(-forward_sum)).astype(kind),
                key_backward=(keys * jnp.exp(-backward_sum)).astype(kind),
                carry_forward=(keys * jnp.exp(rest)).astype(kind),
                carry_backward=(keys * jnp.exp(forward_sum - log_decay)).astype(kind),
            )
        )
    for head in range(head_count):
        lanes = slice(head * KEY_DIM, (head + 1) * KEY_DIM)
        values = [
            rounded(block, 2 * half + head * VALUE_DIM, VALUE_DIM) for block in range(block_count)
        ]

        def states(order, carry):
            running = None
            found = {}
            for block in order:
                found[block] = running
                update = dot(values[block], terms[block][carry][:, lanes], ((0,), (0,)))
                if running is not None:
                    update = running * terms[block]["total"][:, lanes] + update
                running = update
            return found

        before = states(range(block_count), "carry_forward")
        after = states(range(block_count - 1, -1, -1), "carry_backward")
        for block in range(block_count):
            term = {name: value[:, lanes] for name, value in terms[block].items()}
            last = ((1,), (1,))
            weights = jnp.where(lower, dot(term["query_forward"], term["key_forward"], last), 0.0)
            weights = weights + jnp.where(
                upper, dot(term["query_backward"], term["key_backward"], last), 0.0
            )
            result = dot(weights.astype(jnp.bfloat16), values[block], ((1,), (0,)))
            if before[block] is not None:
                result = result + dot(
                    term["query_forward"], before[block].astype(jnp.bfloat16), last
                )
            if after[block] is not None:
                result = result + dot(
                    term["query_backward"], after[block].astype(jnp.bfloat16), last
                )
            scaled = result * lax.rsqrt(
                jnp.mean(result * result, axis=-1, keepdims=True) + norm_eps
            )
            gates = rounded(block, 2 * half + wide + head * VALUE_DIM, VALUE_DIM)
            gates = gates.astype(jnp.float32)
            merged = scaled * gain * (gates / (1.0 + jnp.exp(-gates)))
            out_ref[
                block * BLOCK : (block + 1) * BLOCK, head * VALUE_DIM : (head + 1) * VALUE_DIM
            ] = merged.astype(jnp.bfloat16)


def mixer_heads(projected, added, shift, gain):
    row_count, width = projected.shape
    half = added.shape[1]
    wide = half // KEY_DIM * VALUE_DIM
    return pl.pallas_call(
        attention_kernel,
        grid=(row_count // SEQ_LEN,),
        in_specs=[
            pl.BlockSpec((SEQ_LEN, width), lambda i: (i, 0)),
            pl.BlockSpec((SEQ_LEN, half), lambda i: (i, 0)),
            pl.BlockSpec((1, half), lambda i: (0, 0)),
            pl.BlockSpec((1, VALUE_DIM), lambda i: (0, 0)),
        ],
        out_specs=pl.BlockSpec((SEQ_LEN, wide), lambda i: (i, 0)),
        out_shape=jax.ShapeDtypeStruct((row_count, wide), jnp.bfloat16),
    )(projected, added, shift.reshape(1, -1), gain.reshape(1, -1))

def depthwise(linear_out, gated_out, depthwise_taps, depthwise_bias):
    row_count, channels = linear_out.shape

    def smooth(source, taps, offset_bias):
        framed = source.astype(jnp.float32).reshape(row_count // SEQ_LEN, SEQ_LEN, channels)
        tap_count = taps.shape[0]
        leading_zero_fill = tap_count // 2
        padded = jnp.pad(
            framed, ((0, 0), (leading_zero_fill, tap_count - 1 - leading_zero_fill), (0, 0))
        )
        result = offset_bias.astype(jnp.float32)
        for shift_index in range(tap_count):
            result = result + padded[:, shift_index : shift_index + SEQ_LEN] * taps[
                shift_index
            ].astype(jnp.float32)
        return result

    linear_conv = smooth(linear_out, depthwise_taps[0], depthwise_bias[0])
    gate_conv = smooth(gated_out, depthwise_taps[1], depthwise_bias[1])
    return (linear_conv * jax.nn.silu(gate_conv)).astype(jnp.bfloat16).reshape(row_count, channels)


def other_half(source):
    return lax.ppermute(source, "tp", [(0, 1), (1, 0)])


def both_halves(own, other):
    first = lax.axis_index("tp") == 0
    return jnp.concatenate([jnp.where(first, own, other), jnp.where(first, other, own)], axis=1)


def ring_gather(shard, fs_size, widths, gate):
    row_count, width = shard.shape
    sub = 8
    shard = shard.reshape(row_count // sub, sub, width)
    if gate is not None:
        shard = lax.optimization_barrier((shard, *gate))[0]
    count = row_count // sub
    side = -(-count // 3)
    place = lax.axis_index("fs")
    rep = lax.axis_index("rep")
    pairs = fs_size // 2
    spot = jnp.where(place % 2 == 0, place // 2, fs_size - 1 - place // 2)

    def member(index):
        return 2 * index if index < pairs else 2 * (fs_size - 1 - index) + 1

    def member_at(index):
        index = (index + 2 * fs_size) % fs_size
        return jnp.where(index < pairs, 2 * index, 2 * (fs_size - 1 - index) + 1)

    upward = [(member(i), member((i + 1) % fs_size)) for i in range(fs_size)]
    downward = [(b, a) for a, b in upward]
    starts = [sum(widths[:i]) for i in range(len(widths))]
    gathered = [jnp.zeros((fs_size, count, sub, w), shard.dtype) for w in widths]

    def put(chunk, source, row):
        for i, (start, w) in enumerate(zip(starts, widths)):
            gathered[i] = lax.dynamic_update_slice(
                gathered[i], chunk[None, :, :, start : start + w], (source, row, 0, 0)
            )

    put(shard, place, 0)
    own_row = rep * (count - side)
    other_row = (1 - rep) * (count - side)
    climbing = lax.dynamic_slice_in_dim(shard, own_row, side, 0)
    falling = shard[side : count - side]
    for step in range(1, fs_size):
        climbing = lax.ppermute(climbing, "fs", upward)
        falling = lax.ppermute(falling, "fs", downward)
        handed = lax.ppermute(climbing, "rep", [(0, 1), (1, 0)])
        put(climbing, member_at(spot - step), own_row)
        put(handed, member_at(spot - step), other_row)
        put(falling, member_at(spot + step), side)
    results = [g.reshape(fs_size, row_count, w) for g, w in zip(gathered, widths)]
    return results, (climbing, falling)


def local(
    tokens,
    first_norm_gain,
    query_projection_weight,
    key_projection_weight,
    value_projection_weight,
    output_gate_weight,
    decay_projection_weight,
    fading_shift_vector,
    added_fading_exponent,
    per_head_gain,
    mixer_result_matrix,
    second_norm_gain,
    up_linear_weight,
    up_gating_weight,
    depthwise_taps,
    depthwise_bias,
    down_projection_weight,
    fs_size,
):
    share = query_projection_weight.shape[0]
    first_pack = jnp.concatenate(
        [
            query_projection_weight,
            key_projection_weight,
            value_projection_weight,
            output_gate_weight,
            decay_projection_weight,
        ],
        axis=1,
    )
    mixer_rows, mixer_cols = mixer_result_matrix.shape
    folds = mixer_rows // share
    units = up_linear_weight.shape[1]
    second_pack = jnp.concatenate(
        [up_linear_weight, up_gating_weight]
        + [mixer_result_matrix[i * share : (i + 1) * share] for i in range(folds)],
        axis=1,
    )
    (first_weight,), gate = ring_gather(first_pack, fs_size, (first_pack.shape[1],), None)
    (up_weight, mixer_weight), gate = ring_gather(
        second_pack, fs_size, (2 * units, folds * mixer_cols), gate
    )
    (down_weight,), gate = ring_gather(
        down_projection_weight, fs_size, (down_projection_weight.shape[1],), gate
    )

    whole_rows = both_halves(tokens, other_half(tokens))
    normed = normalize(whole_rows, first_norm_gain)
    width = normed.shape[1]
    projected = jnp.dot(
        normed, first_weight.reshape(width, -1), preferred_element_type=jnp.float32
    )
    mixed_heads = mixer_heads(projected, added_fading_exponent, fading_shift_vector, per_head_gain)
    mixer_weight = mixer_weight.reshape(fs_size, share, folds, mixer_cols)
    mixer_weight = mixer_weight.transpose(2, 1, 0, 3).reshape(mixer_rows, fs_size * mixer_cols)
    mixer_terms = jnp.dot(
        mixed_heads, mixer_weight, preferred_element_type=jnp.float32
    ).astype(jnp.bfloat16)
    summed = mixer_terms.astype(jnp.float32) + other_half(mixer_terms).astype(jnp.float32)
    full_after = (whole_rows.astype(jnp.float32) + summed).astype(jnp.bfloat16)
    feature_share = tokens.shape[1]
    half_index = lax.axis_index("tp")
    after_mixer = lax.dynamic_slice_in_dim(
        full_after, half_index * feature_share, feature_share, 1
    )
    normed_two = normalize(full_after, second_norm_gain)
    upward = jnp.dot(
        normed_two, up_weight.reshape(width, -1), preferred_element_type=jnp.float32
    ).astype(jnp.bfloat16)
    hidden = depthwise(upward[:, :units], upward[:, units:], depthwise_taps, depthwise_bias)
    channel_terms = jnp.concatenate(
        [
            jnp.dot(hidden, down_weight[i], preferred_element_type=jnp.float32)
            for i in range(fs_size)
        ],
        axis=1,
    ).astype(jnp.bfloat16)
    kept = lax.dynamic_slice_in_dim(channel_terms, half_index * feature_share, feature_share, 1)
    sent = lax.dynamic_slice_in_dim(
        channel_terms, (1 - half_index) * feature_share, feature_share, 1
    )
    channel_part = kept.astype(jnp.float32) + other_half(sent).astype(jnp.float32)
    return (after_mixer.astype(jnp.float32) + channel_part).astype(jnp.bfloat16)


def solution(mesh):
    return jax.shard_map(
        functools.partial(local, fs_size=mesh.shape["fs"]),
        mesh=mesh,
        in_specs=(
            P(("rep", "fs"), "tp"),
            P(),
            P("fs", "tp"),
            P("fs", "tp"),
            P("fs", "tp"),
            P("fs", "tp"),
            P("fs", "tp"),
            P("tp"),
            P(("rep", "fs"), "tp"),
            P(),
            P("tp", "fs"),
            P(),
            P("fs", "tp"),
            P("fs", "tp"),
            P(None, None, "tp"),
            P(None, "tp"),
            P("tp", "fs"),
        ),
        out_specs=P(("rep", "fs"), "tp"),
        check_vma=False,
    )
```

```python
import functools

import jax
import jax.numpy as jnp
from jax import lax
from jax.experimental import pallas as pl
from jax.experimental.pallas import tpu as pltpu
from jax.sharding import PartitionSpec as P

KEY_DIM = 64
VALUE_DIM = 128
BLOCK = 64
SEQ_LEN = 256


norm_eps = 1e-06
fading_sharpness = 16.0


def normalize(source, gain):
    widened = source.astype(jnp.float32)
    scaled = widened * lax.rsqrt(jnp.mean(widened * widened, axis=-1, keepdims=True) + norm_eps)
    return (scaled * gain.astype(jnp.float32)).astype(jnp.bfloat16)


def attention_kernel(projected_ref, added_ref, shift_ref, gain_ref, out_ref):
    length, half = added_ref.shape
    head_count = half // KEY_DIM
    wide = head_count * VALUE_DIM
    block_count = length // BLOCK
    rows = lax.broadcasted_iota(jnp.int32, (BLOCK, BLOCK), 0)
    cols = lax.broadcasted_iota(jnp.int32, (BLOCK, BLOCK), 1)
    lower = rows >= cols
    upper = rows <= cols
    ones_lower = lower.astype(jnp.float32)
    gain = gain_ref[...].astype(jnp.float32)
    shift = shift_ref[...]

    def dot(left, right, dims):
        return lax.dot_general(left, right, (dims, ((), ())), preferred_element_type=jnp.float32)

    def rounded(block, start, size):
        part = projected_ref[block * BLOCK : (block + 1) * BLOCK, start : start + size]
        return part.astype(jnp.bfloat16)

    terms = []
    for block in range(block_count):
        span = slice(block * BLOCK, (block + 1) * BLOCK)
        scores = projected_ref[span, 2 * half + 2 * wide :] + shift
        log_decay = (
            jnp.minimum(scores, 0.0) - jnp.log1p(jnp.exp(-jnp.abs(scores)))
        ) / fading_sharpness + added_ref[span, :]
        forward_sum = lax.dot_general(
            ones_lower,
            log_decay,
            (((1,), (0,)), ((), ())),
            precision=lax.Precision.HIGHEST,
            preferred_element_type=jnp.float32,
        )
        total = forward_sum[BLOCK - 1 : BLOCK]
        rest = total - forward_sum
        backward_sum = rest + log_decay
        queries = rounded(block, 0, half).astype(jnp.float32) * KEY_DIM ** (-0.5)
        keys = rounded(block, half, half).astype(jnp.float32)
        kind = jnp.bfloat16
        terms.append(
            dict(
                total=jnp.exp(total),
                query_forward=(queries * jnp.exp(forward_sum)).astype(kind),
                query_backward=(queries * jnp.exp(backward_sum)).astype(kind),
                key_forward=(keys * jnp.exp(-forward_sum)).astype(kind),
                key_backward=(keys * jnp.exp(-backward_sum)).astype(kind),
                carry_forward=(keys * jnp.exp(rest)).astype(kind),
                carry_backward=(keys * jnp.exp(forward_sum - log_decay)).astype(kind),
            )
        )
    for head in range(head_count):
        lanes = slice(head * KEY_DIM, (head + 1) * KEY_DIM)
        values = [
            rounded(block, 2 * half + head * VALUE_DIM, VALUE_DIM) for block in range(block_count)
        ]

        def states(order, carry):
            running = None
            found = {}
            for block in order:
                found[block] = running
                update = dot(values[block], terms[block][carry][:, lanes], ((0,), (0,)))
                if running is not None:
                    update = running * terms[block]["total"][:, lanes] + update
                running = update
            return found

        before = states(range(block_count), "carry_forward")
        after = states(range(block_count - 1, -1, -1), "carry_backward")
        for block in range(block_count):
            term = {name: value[:, lanes] for name, value in terms[block].items()}
            last = ((1,), (1,))
            weights = jnp.where(lower, dot(term["query_forward"], term["key_forward"], last), 0.0)
            weights = weights + jnp.where(
                upper, dot(term["query_backward"], term["key_backward"], last), 0.0
            )
            result = dot(weights.astype(jnp.bfloat16), values[block], ((1,), (0,)))
            if before[block] is not None:
                result = result + dot(
                    term["query_forward"], before[block].astype(jnp.bfloat16), last
                )
            if after[block] is not None:
                result = result + dot(
                    term["query_backward"], after[block].astype(jnp.bfloat16), last
                )
            scaled = result * lax.rsqrt(
                jnp.mean(result * result, axis=-1, keepdims=True) + norm_eps
            )
            gates = rounded(block, 2 * half + wide + head * VALUE_DIM, VALUE_DIM)
            gates = gates.astype(jnp.float32)
            merged = scaled * gain * (gates / (1.0 + jnp.exp(-gates)))
            out_ref[
                block * BLOCK : (block + 1) * BLOCK, head * VALUE_DIM : (head + 1) * VALUE_DIM
            ] = merged.astype(jnp.bfloat16)


def mixer_heads(projected, added, shift, gain):
    row_count, width = projected.shape
    half = added.shape[1]
    wide = half // KEY_DIM * VALUE_DIM
    return pl.pallas_call(
        attention_kernel,
        grid=(row_count // SEQ_LEN,),
        in_specs=[
            pl.BlockSpec((SEQ_LEN, width), lambda i: (i, 0)),
            pl.BlockSpec((SEQ_LEN, half), lambda i: (i, 0)),
            pl.BlockSpec((1, half), lambda i: (0, 0)),
            pl.BlockSpec((1, VALUE_DIM), lambda i: (0, 0)),
        ],
        out_specs=pl.BlockSpec((SEQ_LEN, wide), lambda i: (i, 0)),
        out_shape=jax.ShapeDtypeStruct((row_count, wide), jnp.bfloat16),
    )(projected, added, shift.reshape(1, -1), gain.reshape(1, -1))

def depthwise(linear_out, gated_out, depthwise_taps, depthwise_bias):
    row_count, channels = linear_out.shape

    def smooth(source, taps, offset_bias):
        framed = source.astype(jnp.float32).reshape(row_count // SEQ_LEN, SEQ_LEN, channels)
        tap_count = taps.shape[0]
        leading_zero_fill = tap_count // 2
        padded = jnp.pad(
            framed, ((0, 0), (leading_zero_fill, tap_count - 1 - leading_zero_fill), (0, 0))
        )
        result = offset_bias.astype(jnp.float32)
        for shift_index in range(tap_count):
            result = result + padded[:, shift_index : shift_index + SEQ_LEN] * taps[
                shift_index
            ].astype(jnp.float32)
        return result

    linear_conv = smooth(linear_out, depthwise_taps[0], depthwise_bias[0])
    gate_conv = smooth(gated_out, depthwise_taps[1], depthwise_bias[1])
    return (linear_conv * jax.nn.silu(gate_conv)).astype(jnp.bfloat16).reshape(row_count, channels)


def other_half(source):
    return lax.ppermute(source, "tp", [(0, 1), (1, 0)])


def both_halves(own, other):
    first = lax.axis_index("tp") == 0
    return jnp.concatenate([jnp.where(first, own, other), jnp.where(first, other, own)], axis=1)


def ring_gather(shard, fs_size, widths, gate, hooks=()):
    row_count, width = shard.shape
    sub = 8
    shard = shard.reshape(row_count // sub, sub, width)
    if gate is not None:
        shard = lax.optimization_barrier((shard, *gate))[0]
    count = row_count // sub
    side = -(-count // 3)
    place = lax.axis_index("fs")
    rep = lax.axis_index("rep")
    pairs = fs_size // 2
    spot = jnp.where(place % 2 == 0, place // 2, fs_size - 1 - place // 2)

    def member(index):
        return 2 * index if index < pairs else 2 * (fs_size - 1 - index) + 1

    def member_at(index):
        index = (index + 2 * fs_size) % fs_size
        return jnp.where(index < pairs, 2 * index, 2 * (fs_size - 1 - index) + 1)

    upward = [(member(i), member((i + 1) % fs_size)) for i in range(fs_size)]
    downward = [(b, a) for a, b in upward]
    starts = [sum(widths[:i]) for i in range(len(widths))]
    gathered = [jnp.zeros((fs_size, count, sub, w), shard.dtype) for w in widths]

    def put(chunk, source, row):
        for i, (start, w) in enumerate(zip(starts, widths)):
            gathered[i] = lax.dynamic_update_slice(
                gathered[i], chunk[None, :, :, start : start + w], (source, row, 0, 0)
            )

    put(shard, place, 0)
    own_row = rep * (count - side)
    other_row = (1 - rep) * (count - side)
    climbing = lax.dynamic_slice_in_dim(shard, own_row, side, 0)
    falling = shard[side : count - side]
    early = None
    for step in range(1, fs_size):
        climbing = lax.ppermute(climbing, "fs", upward)
        falling = lax.ppermute(falling, "fs", downward)
        handed = lax.ppermute(climbing, "rep", [(0, 1), (1, 0)])
        put(climbing, member_at(spot - step), own_row)
        put(handed, member_at(spot - step), other_row)
        put(falling, member_at(spot + step), side)
        if step == max(1, fs_size - 1 - 0):
            early = (climbing, falling)
        for when, value in hooks:
            if step == when:
                climbing, falling, _ = lax.optimization_barrier((climbing, falling, value))
    results = [g.reshape(fs_size, row_count, w) for g, w in zip(gathered, widths)]
    return results, early


def local(
    tokens,
    first_norm_gain,
    query_projection_weight,
    key_projection_weight,
    value_projection_weight,
    output_gate_weight,
    decay_projection_weight,
    fading_shift_vector,
    added_fading_exponent,
    per_head_gain,
    mixer_result_matrix,
    second_norm_gain,
    up_linear_weight,
    up_gating_weight,
    depthwise_taps,
    depthwise_bias,
    down_projection_weight,
    fs_size,
):
    share = query_projection_weight.shape[0]
    mixer_rows, mixer_cols = mixer_result_matrix.shape
    folds = mixer_rows // share
    units = up_linear_weight.shape[1]
    projections = jnp.concatenate(
        [
            query_projection_weight,
            key_projection_weight,
            value_projection_weight,
            output_gate_weight,
            decay_projection_weight,
        ],
        axis=1,
    )
    first_pack = jnp.concatenate(
        [projections]
        + [mixer_result_matrix[i * share : (i + 1) * share] for i in range(folds)],
        axis=1,
    )
    second_pack = jnp.concatenate([up_linear_weight, up_gating_weight], axis=1)
    (first_weight, mixer_weight), gate = ring_gather(
        first_pack, fs_size, (projections.shape[1], folds * mixer_cols), None
    )
    (up_weight,), gate = ring_gather(second_pack, fs_size, (2 * units,), gate)

    whole_rows = both_halves(tokens, other_half(tokens))
    normed = normalize(whole_rows, first_norm_gain)
    width = normed.shape[1]
    projected = jnp.dot(
        normed, first_weight.reshape(width, -1), preferred_element_type=jnp.float32
    )
    mixed_heads = mixer_heads(projected, added_fading_exponent, fading_shift_vector, per_head_gain)
    mixer_weight = mixer_weight.reshape(fs_size, share, folds, mixer_cols)
    mixer_weight = mixer_weight.transpose(2, 1, 0, 3).reshape(mixer_rows, fs_size * mixer_cols)
    mixer_terms = jnp.dot(
        mixed_heads, mixer_weight, preferred_element_type=jnp.float32
    ).astype(jnp.bfloat16)
    summed = mixer_terms.astype(jnp.float32) + other_half(mixer_terms).astype(jnp.float32)
    full_after = (whole_rows.astype(jnp.float32) + summed).astype(jnp.bfloat16)
    feature_share = tokens.shape[1]
    half_index = lax.axis_index("tp")
    after_mixer = lax.dynamic_slice_in_dim(
        full_after, half_index * feature_share, feature_share, 1
    )
    normed_two = normalize(full_after, second_norm_gain)
    upward = jnp.dot(
        normed_two, up_weight.reshape(width, -1), preferred_element_type=jnp.float32
    ).astype(jnp.bfloat16)
    hidden = depthwise(upward[:, :units], upward[:, units:], depthwise_taps, depthwise_bias)
    (down_weight,), _ = ring_gather(
        down_projection_weight,
        fs_size,
        (down_projection_weight.shape[1],),
        gate,
        ((2, upward), (4, hidden)),
    )
    channel_terms = jnp.concatenate(
        [
            jnp.dot(hidden, down_weight[i], preferred_element_type=jnp.float32)
            for i in range(fs_size)
        ],
        axis=1,
    ).astype(jnp.bfloat16)
    kept = lax.dynamic_slice_in_dim(channel_terms, half_index * feature_share, feature_share, 1)
    sent = lax.dynamic_slice_in_dim(
        channel_terms, (1 - half_index) * feature_share, feature_share, 1
    )
    channel_part = kept.astype(jnp.float32) + other_half(sent).astype(jnp.float32)
    return (after_mixer.astype(jnp.float32) + channel_part).astype(jnp.bfloat16)


def solution(mesh):
    return jax.shard_map(
        functools.partial(local, fs_size=mesh.shape["fs"]),
        mesh=mesh,
        in_specs=(
            P(("rep", "fs"), "tp"),
            P(),
            P("fs", "tp"),
            P("fs", "tp"),
            P("fs", "tp"),
            P("fs", "tp"),
            P("fs", "tp"),
            P("tp"),
            P(("rep", "fs"), "tp"),
            P(),
            P("tp", "fs"),
            P(),
            P("fs", "tp"),
            P("fs", "tp"),
            P(None, None, "tp"),
            P(None, "tp"),
            P("tp", "fs"),
        ),
        out_specs=P(("rep", "fs"), "tp"),
        check_vma=False,
    )
```
